128 devices in a mesh: rep: 2 (over z_hi), fs: 32 (over z_lo, y, x), tp: 2 (over core).
Axes of the slice: x: 4, y: 4, z: 4 (z_hi: 2, z_lo: 2; z = z_hi * 2 + z_lo), core: 2. Of those that a mesh axis runs over, the one named last changes fastest.
Arguments:
- tokens: bfloat16 [65536, 2048], P(('rep', 'fs', 'tp')), parts along dimension 0, may hold values from -6 to 6
- mix_gain: float32 [2048], replicated, may hold values from 0.1 to 1.9
- w_query: bfloat16 [2048, 512], P('fs', 'tp'), may hold values from -0.125 to 0.125
- w_key: bfloat16 [2048, 512], P('fs', 'tp'), may hold values from -0.125 to 0.125
- w_value: bfloat16 [2048, 1024], P('fs', 'tp'), may hold values from -0.125 to 0.125
- w_out: bfloat16 [1024, 2048], P('tp', 'fs'), may hold values from -0.1875 to 0.1875
- ffn_gain: float32 [2048], replicated, may hold values from 0.1 to 1.9
- w_ffgate: bfloat16 [2048, 2816], P('fs', 'tp'), may hold values from -0.125 to 0.125
- w_ffup: bfloat16 [2048, 2816], P('fs', 'tp'), may hold values from -0.125 to 0.125
- conv_gate: float32 [3, 2816], replicated, may hold values from -3 to 3
- conv_up: float32 [3, 2816], replicated, may hold values from -3 to 3
- w_down: bfloat16 [2816, 2048], P('tp', 'fs'), may hold values from -0.109375 to 0.109375
Outputs:
- layer_out: bfloat16 [65536, 2048], P(('rep', 'fs', 'tp')), parts along dimension 0
The draws below stay inside these ranges and needn't reach their ends.
There are 2 independent parts, one for each index of `rep`. The reference program is written for one: setup_inputs(seed, part) draws one part's arguments, and reference() takes and returns one part's arrays. A program takes and returns all parts, laid end to end along the dimension named above; an argument that names none is the same for every part. Nothing has to cross between parts.
All inputs are finite; a program needn't handle non-finite values.
Results may differ from the reference program's by a relative error of at most 0.014.
Values may be sent and summed in bfloat16 or wider, within the bound.
No kernel may reach another device: no remote copies, remote signals or barrier semaphores. Data moves between devices by JAX's collectives and lax.ppermute only.
A program may use at most 128 MiB of HBM per device.

```python
import jax
import jax.numpy as jnp
from jax import lax

D = 2048
HEADS = 4
DK = 128
DV = 256
FF = 2816
KERNEL = 3
BLOCK = 128
LENGTH = 1024
TOKENS = 32768
N_TP = 2


def levels(key, shape, split, low, largest):
    level, own = 1.0, jax.random.fold_in(key, 6)
    for position, shards_of in split:
        draws = jnp.exp(jax.random.uniform(jax.random.fold_in(own, position), (shards_of,), jnp.float32, low / len(split), largest / len(split)))
        level = level * jnp.repeat(draws, shape[position] // shards_of).reshape([-1 if axis == position else 1 for axis in range(len(shape))])
    return level


def bell_draw(key, dims, scale, most, shards=(), kind=jnp.bfloat16):
    level = levels(key, dims, shards, -0.22, 0.18) if shards else 1.0
    drawn = jax.random.normal(key, dims, jnp.float32) * scale * level
    return jnp.minimum(jnp.maximum(drawn, -most), most).astype(kind)


def setup_inputs(seed: int = 0, part: int = 0) -> dict:
    arg_keys = jax.random.split(jax.random.key(seed), 13)
    part_keys = jax.random.split(jax.random.fold_in(arg_keys[12], part), 13)
    return {
        "tokens": bell_draw(part_keys[0], (TOKENS, D), 1.0, 6.0, ((0, 64),)),
        "mix_gain": jnp.clip(1.0 + 0.18 * jax.random.normal(arg_keys[1], (D,), jnp.float32), 0.1, 1.9),
        "w_query": bell_draw(arg_keys[2], (D, HEADS * DK), D ** -0.5, 0.125, ((0, 32), (1, 2))),
        "w_key": bell_draw(arg_keys[3], (D, HEADS * DK), D ** -0.5, 0.125, ((0, 32), (1, 2))),
        "w_value": bell_draw(arg_keys[4], (D, HEADS * DV), D ** -0.5, 0.125, ((0, 32), (1, 2))),
        "w_out": bell_draw(arg_keys[5], (HEADS * DV, D), (HEADS * DV) ** -0.5, 0.1875, ((0, 2), (1, 32))),
        "ffn_gain": jnp.clip(1.0 + 0.18 * jax.random.normal(arg_keys[6], (D,), jnp.float32), 0.1, 1.9),
        "w_ffgate": bell_draw(arg_keys[7], (D, FF), D ** -0.5, 0.125, ((0, 32), (1, 2))),
        "w_ffup": bell_draw(arg_keys[8], (D, FF), D ** -0.5, 0.125, ((0, 32), (1, 2))),
        "conv_gate": bell_draw(arg_keys[9], (KERNEL, FF), 0.58, 3.0, (), jnp.float32),
        "conv_up": bell_draw(arg_keys[10], (KERNEL, FF), 0.58, 3.0, (), jnp.float32),
        "w_down": bell_draw(arg_keys[11], (FF, D), FF ** -0.5, 0.109375, ((0, 2), (1, 32))),
    }


epsilon = 1e-06

def rms_rows(matrix, scale_vec):
    values = matrix.astype(jnp.float32)
    factor = lax.rsqrt(lax.optimization_barrier(jnp.mean(values * values, axis=-1, keepdims=True)) + epsilon)
    return (values * factor * scale_vec).astype(jnp.bfloat16)

def rotate_heads(matrix):
    length = matrix.shape[0]
    half_width = matrix.shape[-1] // 2
    inverse = 10000.0 ** (-jnp.arange(half_width, dtype=jnp.float32) * 2.0 / (2 * half_width))
    angles = jnp.arange(length, dtype=jnp.float32)[:, None] * inverse[None, :]
    cosine = jnp.cos(angles)[:, None, :]
    sine = jnp.sin(angles)[:, None, :]
    values = matrix.astype(jnp.float32)
    first_half = values[..., :half_width]
    second_half = values[..., half_width:]
    return jnp.concatenate([first_half * cosine - second_half * sine, first_half * sine + second_half * cosine], axis=-1)

def retain_blocks(rot_query, rot_key, value, rates, block_len):
    length, head_count, width_k = rot_query.shape
    width_v = value.shape[-1]
    blocks = length // block_len
    query4 = rot_query.reshape(blocks, block_len, head_count, width_k).astype(jnp.float32)
    key4 = rot_key.reshape(blocks, block_len, head_count, width_k)
    value4 = value.reshape(blocks, block_len, head_count, width_v).astype(jnp.float32)
    places = jnp.arange(block_len, dtype=jnp.float32)
    spacing = places[:, None] - places[None, :]
    inside = jnp.where(spacing[None] >= 0, jnp.exp(-jnp.maximum(spacing, 0.0)[None] * rates[:, None, None]), 0.0)
    scores = jnp.einsum('cihd,cjhd->chij', query4, key4.astype(jnp.float32), precision=lax.Precision.HIGHEST)
    weights = (scores * inside[None]).astype(jnp.bfloat16)
    inner_part = jnp.einsum('chij,cjhe->cihe', weights.astype(jnp.float32), value4, precision=lax.Precision.HIGHEST)
    tail_decay = jnp.exp(-(block_len - 1.0 - places)[:, None] * rates[None, :])
    decayed = (key4.astype(jnp.float32) * tail_decay[None, :, :, None]).astype(jnp.bfloat16)
    states = jnp.einsum('cjhd,cjhe->chde', decayed.astype(jnp.float32), value4, precision=lax.Precision.HIGHEST)
    passing = jnp.exp(-block_len * rates)[:, None, None]

    def advance(carried, fresh):
        return (carried * passing + fresh, carried)
    _, before = lax.scan(advance, jnp.zeros((head_count, width_k, width_v), jnp.float32), states)
    onset_decay = jnp.exp(-(places + 1.0)[:, None] * rates[None, :])
    cross_part = jnp.einsum('cihd,chde->cihe', query4, before, precision=lax.Precision.HIGHEST) * onset_decay[None, :, :, None]
    return (inner_part + cross_part).reshape(length, head_count, width_v)

def head_norm(retained):
    average = lax.optimization_barrier(jnp.mean(retained, axis=-1, keepdims=True))
    centered = retained - average
    return centered * lax.rsqrt(lax.optimization_barrier(jnp.mean(centered * centered, axis=-1, keepdims=True)) + epsilon)

def group_sum(hidden, weight):
    width = hidden.shape[1] // N_TP
    total = jnp.zeros((hidden.shape[0], weight.shape[1]), jnp.float32)
    for section in range(N_TP):
        partial_sum = jnp.dot(hidden[:, section * width:(section + 1) * width], weight[section * width:(section + 1) * width], preferred_element_type=jnp.float32).astype(jnp.bfloat16)
        partial_sum = lax.optimization_barrier(partial_sum)
        total = total + partial_sum.astype(jnp.float32)
    return total

def causal_taps(matrix, kernel_w):
    length = matrix.shape[0]
    padded = jnp.pad(matrix.astype(jnp.float32), ((KERNEL - 1, 0), (0, 0)))
    total = jnp.zeros((length, matrix.shape[1]), jnp.float32)
    for tap_idx in range(KERNEL):
        total = total + kernel_w[tap_idx][None, :] * padded[tap_idx:tap_idx + length]
    return total

def reference(tokens, mix_gain, w_query, w_key, w_value, w_out, ffn_gain, w_ffgate, w_ffup, conv_gate, conv_up, w_down):
    sequences = tokens.reshape(TOKENS // LENGTH, LENGTH, D)

    def layer(rows):
        normed = rms_rows(rows, mix_gain)
        query = jnp.dot(normed, w_query, preferred_element_type=jnp.float32).astype(jnp.bfloat16)
        key = jnp.dot(normed, w_key, preferred_element_type=jnp.float32).astype(jnp.bfloat16)
        value = jnp.dot(normed, w_value, preferred_element_type=jnp.float32).astype(jnp.bfloat16)
        rot_query = rotate_heads(query.reshape(LENGTH, HEADS, DK)).astype(jnp.bfloat16)
        rot_key = (rotate_heads(key.reshape(LENGTH, HEADS, DK)) * DK ** (-0.5)).astype(jnp.bfloat16)
        rates = 1.0 / 16.0 * (32.0 / LENGTH) ** (jnp.arange(HEADS, dtype=jnp.float32) / (HEADS - 1))
        retained = retain_blocks(rot_query, rot_key, value.reshape(LENGTH, HEADS, DV), rates, BLOCK)
        hidden = head_norm(retained).reshape(LENGTH, HEADS * DV).astype(jnp.bfloat16)
        mix_sum = group_sum(hidden, w_out)
        resid = (rows.astype(jnp.float32) + mix_sum).astype(jnp.bfloat16)
        normed_ffn = rms_rows(resid, ffn_gain)
        gate_pre = jnp.dot(normed_ffn, w_ffgate, preferred_element_type=jnp.float32).astype(jnp.bfloat16)
        up_pre = jnp.dot(normed_ffn, w_ffup, preferred_element_type=jnp.float32).astype(jnp.bfloat16)
        activ = (jax.nn.silu(causal_taps(gate_pre, conv_gate)) * causal_taps(up_pre, conv_up)).astype(jnp.bfloat16)
        ffn_sum = group_sum(activ, w_down)
        return (resid.astype(jnp.float32) + ffn_sum).astype(jnp.bfloat16)
    return lax.map(layer, sequences).reshape(TOKENS, D)
```

```python
import jax
import jax.numpy as jnp
from jax import lax
from jax.sharding import Mesh
from jax.sharding import PartitionSpec as P

HEADS = 4
DK = 128
DV = 256
KERNEL = 3
BLOCK = 128
LENGTH = 1024


epsilon = 1e-06


def ring(size, step):
    return [(i, (i + step) % size) for i in range(size)]


def shift(v, axis, step):
    return lax.ppermute(v, axis, ring(lax.axis_size(axis), step))


def placed_at(parts, index, dim):
    first = parts[0][1]
    shape = list(first.shape)
    shape.insert(dim, len(parts))
    buf = jnp.zeros(shape, first.dtype)
    for pos, block in parts:
        buf = lax.dynamic_update_slice_in_dim(buf, jnp.expand_dims(block, dim), pos, dim)
    return buf


def ring4_direct(block, axis, dim):
    me = lax.axis_index(axis)
    left = shift(block, axis, 1)
    right = shift(block, axis, -1)
    far = shift(block, axis, 2)
    return placed_at(
        [(me, block), ((me + 3) % 4, left), ((me + 1) % 4, right), ((me + 2) % 4, far)], me, dim
    )


def ring4_forward(block, axis, dim):
    me = lax.axis_index(axis)
    left = shift(block, axis, 1)
    right = shift(block, axis, -1)
    far0 = shift(left[:1], axis, 1)
    far1 = shift(right[1:], axis, -1)
    far = jnp.concatenate([far0, far1], axis=0)
    return placed_at(
        [(me, block), ((me + 3) % 4, left), ((me + 1) % 4, right), ((me + 2) % 4, far)], me, dim
    )


def gather_two(a, b):
    na = a.shape[1]
    both = jnp.concatenate([a, b], axis=1)
    other = shift(both, "z", 1)
    z = lax.axis_index("z")
    pair = placed_at([(z, both), (1 - z, other)], z, 0)
    block_a, block_b = pair[:, :, :na], pair[:, :, na:]
    block_a = ring4_direct(block_a, "x", 1)
    block_b = ring4_direct(block_b, "y", 1)
    full_a = ring4_forward(block_a, "y", 1)
    full_b = ring4_forward(block_b, "x", 2)
    return full_a.reshape(-1, na), full_b.reshape(-1, b.shape[1])


def both_rows(rows):
    me = lax.axis_index("tp")
    other = shift(rows, "tp", 1)
    return lax.dynamic_update_slice_in_dim(
        lax.dynamic_update_slice_in_dim(
            jnp.zeros((2 * rows.shape[0], rows.shape[1]), rows.dtype), rows, me * rows.shape[0], 0
        ),
        other,
        (1 - me) * rows.shape[0],
        0,
    )


def sum_rows(partial):
    me = lax.axis_index("tp")
    half = partial.shape[0] // 2
    mine = lax.dynamic_slice_in_dim(partial, me * half, half, 0)
    theirs = lax.dynamic_slice_in_dim(partial, (1 - me) * half, half, 0)
    got = shift(theirs, "tp", 1)
    return mine.astype(jnp.float32) + got.astype(jnp.float32)


def rms_rows(matrix, scale_vec):
    values = matrix.astype(jnp.float32)
    factor = lax.rsqrt(jnp.mean(values * values, axis=-1, keepdims=True) + epsilon)
    return (values * factor * scale_vec).astype(jnp.bfloat16)


def rotate_heads(matrix):
    length = matrix.shape[0]
    half_width = matrix.shape[-1] // 2
    inverse = 10000.0 ** (-jnp.arange(half_width, dtype=jnp.float32) * 2.0 / (2 * half_width))
    angles = jnp.arange(length, dtype=jnp.float32)[:, None] * inverse[None, :]
    cosine = jnp.cos(angles)[:, None, :]
    sine = jnp.sin(angles)[:, None, :]
    values = matrix.astype(jnp.float32)
    first_half = values[..., :half_width]
    second_half = values[..., half_width:]
    return jnp.concatenate(
        [first_half * cosine - second_half * sine, first_half * sine + second_half * cosine],
        axis=-1,
    )


def retain_blocks(rot_query, rot_key, value, rates, block_len):
    length, head_count, width_k = rot_query.shape
    width_v = value.shape[-1]
    blocks = length // block_len
    query4 = rot_query.reshape(blocks, block_len, head_count, width_k)
    key4 = rot_key.reshape(blocks, block_len, head_count, width_k)
    value4 = value.reshape(blocks, block_len, head_count, width_v)
    places = jnp.arange(block_len, dtype=jnp.float32)
    spacing = places[:, None] - places[None, :]
    inside = jnp.where(
        spacing[None] >= 0, jnp.exp(-jnp.maximum(spacing, 0.0)[None] * rates[:, None, None]), 0.0
    )
    scores = jnp.einsum("cihd,cjhd->chij", query4, key4, preferred_element_type=jnp.float32)
    weights = (scores * inside[None]).astype(jnp.bfloat16)
    inner_part = jnp.einsum("chij,cjhe->cihe", weights, value4, preferred_element_type=jnp.float32)
    tail_decay = jnp.exp(-(block_len - 1.0 - places)[:, None] * rates[None, :])
    decayed = (key4.astype(jnp.float32) * tail_decay[None, :, :, None]).astype(jnp.bfloat16)
    states = jnp.einsum("cjhd,cjhe->chde", decayed, value4, preferred_element_type=jnp.float32)
    passing = jnp.exp(-block_len * rates)[:, None, None]

    def advance(carried, fresh):
        return (carried * passing + fresh, carried)

    _, before = lax.scan(advance, jnp.zeros((head_count, width_k, width_v), jnp.float32), states)
    onset_decay = jnp.exp(-(places + 1.0)[:, None] * rates[None, :])
    cross_part = (
        jnp.einsum("cihd,chde->cihe", query4.astype(jnp.float32), before)
        * onset_decay[None, :, :, None]
    )
    return (inner_part + cross_part).reshape(length, head_count, width_v)


def head_norm(retained):
    average = jnp.mean(retained, axis=-1, keepdims=True)
    centered = retained - average
    return centered * lax.rsqrt(jnp.mean(centered * centered, axis=-1, keepdims=True) + epsilon)


def causal_taps(matrix, kernel_w):
    length = matrix.shape[0]
    padded = jnp.pad(matrix.astype(jnp.float32), ((KERNEL - 1, 0), (0, 0)))
    total = jnp.zeros((length, matrix.shape[1]), jnp.float32)
    for tap_idx in range(KERNEL):
        total = total + kernel_w[tap_idx][None, :] * padded[tap_idx : tap_idx + length]
    return total


def body(
    tokens,
    mix_gain,
    w_query,
    w_key,
    w_value,
    w_out,
    ffn_gain,
    w_ffgate,
    w_ffup,
    conv_gate,
    conv_up,
    w_down,
):
    tp_rank = lax.axis_index("tp")
    heads_here = w_query.shape[1] // DK
    normed = rms_rows(tokens, mix_gain)
    w_qk, w_v = gather_two(jnp.concatenate([w_query, w_key], axis=1), w_value)
    out_t = w_out.T
    half_out = out_t.shape[1] // 2
    out_a, out_b = gather_two(out_t[:, :half_out], out_t[:, half_out:])
    gate_w, up_w = gather_two(w_ffgate, w_ffup)
    down_t = w_down.T
    down_a, down_b = gather_two(down_t[:, :768], down_t[:, 768:])
    pieces = both_rows(normed)
    qk = jnp.dot(pieces, w_qk, preferred_element_type=jnp.float32).astype(jnp.bfloat16)
    value = jnp.dot(pieces, w_v, preferred_element_type=jnp.float32).astype(jnp.bfloat16)
    qk_cols = w_query.shape[1]
    length = pieces.shape[0]
    query = qk[:, :qk_cols].reshape(length, heads_here, DK)
    key = qk[:, qk_cols:].reshape(length, heads_here, DK)
    value = value.reshape(length, heads_here, DV)
    rot_query = rotate_heads(query).astype(jnp.bfloat16)
    rot_key = (rotate_heads(key) * DK ** (-0.5)).astype(jnp.bfloat16)
    head_ids = (tp_rank * heads_here + jnp.arange(heads_here, dtype=jnp.int32)).astype(jnp.float32)
    rates = 1.0 / 16.0 * (32.0 / LENGTH) ** (head_ids / (HEADS - 1))
    retained = retain_blocks(rot_query, rot_key, value, rates, BLOCK)
    hidden = head_norm(retained).reshape(length, heads_here * DV).astype(jnp.bfloat16)
    nt = (((1,), (1,)), ((), ()))
    mix = lax.dot_general(
        hidden, jnp.concatenate([out_a, out_b], axis=1), nt, preferred_element_type=jnp.float32
    ).astype(jnp.bfloat16)
    mix_sum = sum_rows(mix)
    resid = (tokens.astype(jnp.float32) + mix_sum).astype(jnp.bfloat16)
    normed_ffn = rms_rows(resid, ffn_gain)
    ff_here = w_ffgate.shape[1]
    pieces = both_rows(normed_ffn)
    gate_pre = jnp.dot(pieces, gate_w, preferred_element_type=jnp.float32).astype(jnp.bfloat16)
    up_pre = jnp.dot(pieces, up_w, preferred_element_type=jnp.float32).astype(jnp.bfloat16)
    gate_taps = lax.dynamic_slice_in_dim(conv_gate, tp_rank * ff_here, ff_here, 1)
    up_taps = lax.dynamic_slice_in_dim(conv_up, tp_rank * ff_here, ff_here, 1)
    activ = (jax.nn.silu(causal_taps(gate_pre, gate_taps)) * causal_taps(up_pre, up_taps)).astype(
        jnp.bfloat16
    )
    ffn = lax.dot_general(
        activ, jnp.concatenate([down_a, down_b], axis=1), nt, preferred_element_type=jnp.float32
    ).astype(jnp.bfloat16)
    ffn_sum = sum_rows(ffn)
    return (resid.astype(jnp.float32) + ffn_sum).astype(jnp.bfloat16)


def solution(mesh):
    torus = Mesh(mesh.devices.reshape(2, 2, 4, 4, 2), ("rep", "z", "y", "x", "tp"))
    fs = ("z", "y", "x")
    rows = P(("rep", *fs, "tp"), None)
    placed = (
        rows,
        P(),
        P(fs, "tp"),
        P(fs, "tp"),
        P(fs, "tp"),
        P("tp", fs),
        P(),
        P(fs, "tp"),
        P(fs, "tp"),
        P(),
        P(),
        P("tp", fs),
    )
    return jax.shard_map(body, mesh=torus, in_specs=placed, out_specs=rows, check_vma=False)
```

```python
import jax
import jax.numpy as jnp
from jax import lax
from jax.experimental import pallas as pl
from jax.experimental.pallas import tpu as pltpu
from jax.sharding import Mesh
from jax.sharding import PartitionSpec as P

HEADS = 4
DK = 128
DV = 256
KERNEL = 3
BLOCK = 128
LENGTH = 1024


epsilon = 1e-06
NT = (((1,), (1,)), ((), ()))
TN = (((0,), (0,)), ((), ()))
FULL = ("rep", "z", "y", "x")


def ring(size, step):
    return [(i, (i + step) % size) for i in range(size)]


def shift(v, axis, step):
    return lax.ppermute(v, axis, ring(lax.axis_size(axis), step))


def lay_out(moves, shapes, where, operands, name):
    hbm = pl.BlockSpec(memory_space=pltpu.MemorySpace.HBM)
    count = len(operands)

    def kernel(where_ref, *refs):
        ins, outs, sems = refs[:count], refs[count:-1], refs[-1]
        copies = [
            pltpu.make_async_copy(src, dst, sems.at[i])
            for i, (src, dst) in enumerate(moves(where_ref, ins, outs))
        ]
        for c in copies:
            c.start()
        for c in copies:
            c.wait()

    return pl.pallas_call(
        kernel,
        out_shape=[jax.ShapeDtypeStruct(shape, jnp.bfloat16) for shape in shapes],
        in_specs=[pl.BlockSpec(memory_space=pltpu.MemorySpace.SMEM)] + [hbm] * count,
        out_specs=[hbm] * len(shapes),
        scratch_shapes=[pltpu.SemaphoreType.DMA((16,))],
        name=name,
    )(where, *operands)


def ring4_direct(block, axis):
    return block, shift(block, axis, 1), shift(block, axis, -1), shift(block, axis, 2)


def ring4_forward(block, axis):
    left = shift(block, axis, 1)
    right = shift(block, axis, -1)
    far0 = shift(left[:1], axis, 1)
    far1 = shift(right[1:], axis, -1)
    return block, left, right, far0, far1


def gather_pieces(both, na, where):
    nb = both.shape[1] - na
    other = shift(both, "z", 1)

    def pair_moves(where_ref, ins, outs):
        z = where_ref[0]
        return [
            (ins[i].at[:, cols], out.at[z if i == 0 else 1 - z])
            for out, cols in ((outs[0], pl.ds(0, na)), (outs[1], pl.ds(na, nb)))
            for i in (0, 1)
        ]

    block_a, block_b = lay_out(
        pair_moves, [(2, 64, na), (2, 64, nb)], where, [both, other], "lay_pair"
    )
    pieces = ring4_direct(block_a, "x") + ring4_direct(block_b, "y")

    def plane_moves(where_ref, ins, outs):
        y, x = where_ref[1], where_ref[2]
        hops = (0, 3, 1, 2)
        return [(ins[i], outs[0].at[:, (x + hops[i]) % 4]) for i in range(4)] + [
            (ins[4 + i], outs[1].at[:, (y + hops[i]) % 4]) for i in range(4)
        ]

    block_a, block_b = lay_out(
        plane_moves, [(2, 4, 64, na), (2, 4, 64, nb)], where, pieces, "lay_plane"
    )
    return ring4_forward(block_a, "y"), ring4_forward(block_b, "x")


def both_rows(rows, where):
    other = shift(rows, "tp", 1)

    def moves(where_ref, ins, outs):
        me = where_ref[3]
        return [(ins[0], outs[0].at[me]), (ins[1], outs[0].at[1 - me])]

    (buf,) = lay_out(moves, [(2, *rows.shape)], where, [rows, other], "lay_rows")
    return buf.reshape(-1, rows.shape[1])


def rms_rows(matrix, scale_vec):
    values = matrix.astype(jnp.float32)
    factor = lax.rsqrt(jnp.mean(values * values, axis=-1, keepdims=True) + epsilon)
    return (values * factor * scale_vec).astype(jnp.bfloat16)


def rotary_tables():
    half_width = DK // 2
    inverse = 10000.0 ** (-jnp.arange(half_width, dtype=jnp.float32) * 2.0 / DK)
    angles = jnp.arange(LENGTH, dtype=jnp.float32)[:, None] * inverse[None, :]
    cosine = jnp.cos(angles)
    sine = jnp.sin(angles)
    return jnp.concatenate([cosine, cosine], axis=1), jnp.concatenate([-sine, sine], axis=1)


def decay_tables(tp_rank, heads_here):
    head_ids = (tp_rank * heads_here + jnp.arange(heads_here, dtype=jnp.int32)).astype(jnp.float32)
    rates = 1.0 / 16.0 * (32.0 / LENGTH) ** (head_ids / (HEADS - 1))
    places = jnp.arange(BLOCK, dtype=jnp.float32)
    spacing = places[:, None] - places[None, :]
    inside = jnp.where(
        spacing[None] >= 0, jnp.exp(-jnp.maximum(spacing, 0.0)[None] * rates[:, None, None]), 0.0
    )
    tail = jnp.exp(-(BLOCK - 1.0 - places)[None, :] * rates[:, None])
    onset = jnp.exp(-(places + 1.0)[None, :] * rates[:, None])
    passing = jnp.exp(-BLOCK * rates)
    tail = jnp.broadcast_to(tail[:, :, None], (heads_here, BLOCK, DK))
    onset = jnp.broadcast_to(onset[:, :, None], (heads_here, BLOCK, DV))
    passing = jnp.broadcast_to(passing[:, None, None], (heads_here, 8, DV))
    return inside, tail, onset, passing


ROWS = 256


def mix_body(
    where_ref, x_ref, cos_ref, sin_ref, inside_ref, tail_ref, onset_ref, passing_ref, *rest
):
    a_own, a_left, a_right, a_far0, a_far1, b_own, b_left, b_right, b_far0, b_far1 = rest[:10]
    out_ref = rest[10]
    wa, wb, carried, sems = rest[11:]
    step = pl.program_id(0)

    @pl.when(step == 0)
    def _():
        y = where_ref[1]
        x = where_ref[2]
        y_left, y_right, y_far = (y + 3) % 4, (y + 1) % 4, (y + 2) % 4
        x_left, x_right, x_far = (x + 3) % 4, (x + 1) % 4, (x + 2) % 4
        moves = [
            (a_own, wa.at[:, y]),
            (a_left, wa.at[:, y_left]),
            (a_right, wa.at[:, y_right]),
            (a_far0.at[0], wa.at[0, y_far]),
            (a_far1.at[0], wa.at[1, y_far]),
            (b_own, wb.at[:, :, x]),
            (b_left, wb.at[:, :, x_left]),
            (b_right, wb.at[:, :, x_right]),
            (b_far0.at[0], wb.at[0, :, x_far]),
            (b_far1.at[0], wb.at[1, :, x_far]),
        ]
        copies = [
            pltpu.make_async_copy(src, dst, sems.at[i]) for i, (src, dst) in enumerate(moves)
        ]
        for c in copies:
            c.start()
        carried[...] = jnp.zeros_like(carried)
        for c in copies:
            c.wait()

    d = x_ref.shape[1]
    heads = 2
    qk_cols = 2 * heads * DK
    v_cols = heads * DV
    x_rows = x_ref[...]
    w_qk = wa[:, :, :, :, :qk_cols].reshape(d, qk_cols)
    w_v = wb[:, :, :, :, :v_cols].reshape(d, v_cols)
    qk = jnp.dot(x_rows, w_qk, preferred_element_type=jnp.float32).astype(jnp.bfloat16)
    value = jnp.dot(x_rows, w_v, preferred_element_type=jnp.float32).astype(jnp.bfloat16)
    cosine = cos_ref[...]
    sine = sin_ref[...]

    def rotary(u):
        u = u.astype(jnp.float32)
        return u * cosine + pltpu.roll(u, DK // 2, 1) * sine

    hidden = []
    for h in range(heads):
        rot_q = rotary(qk[:, h * DK : (h + 1) * DK]).astype(jnp.bfloat16)
        rot_k = (
            rotary(qk[:, (heads + h) * DK : (heads + h + 1) * DK]) * DK ** (-0.5)
        ).astype(jnp.bfloat16)
        v_head = value[:, h * DV : (h + 1) * DV]
        state = carried[h]
        pieces = []
        for c in range(ROWS // BLOCK):
            rows = slice(c * BLOCK, (c + 1) * BLOCK)
            q, k, v = rot_q[rows], rot_k[rows], v_head[rows]
            scores = lax.dot_general(q, k, NT, preferred_element_type=jnp.float32)
            weights = (scores * inside_ref[h]).astype(jnp.bfloat16)
            inner = jnp.dot(weights, v, preferred_element_type=jnp.float32)
            cross = (
                jnp.dot(q, state.astype(jnp.bfloat16), preferred_element_type=jnp.float32)
                * onset_ref[h]
            )
            decayed = (k.astype(jnp.float32) * tail_ref[h]).astype(jnp.bfloat16)
            fresh = lax.dot_general(decayed, v, TN, preferred_element_type=jnp.float32)
            state = state * passing_ref[h, 0:1] + fresh
            retained = inner + cross
            centered = retained - jnp.mean(retained, axis=-1, keepdims=True)
            factor = lax.rsqrt(jnp.mean(centered * centered, axis=-1, keepdims=True) + epsilon)
            pieces.append((centered * factor).astype(jnp.bfloat16))
        carried[h] = state
        hidden.append(jnp.concatenate(pieces, axis=0))
    out_a = wa[:, :, :, :, qk_cols:].reshape(d, DV)
    out_b = wb[:, :, :, :, v_cols:].reshape(d, DV)
    mixed = lax.dot_general(hidden[0], out_a, NT, preferred_element_type=jnp.float32)
    mixed = mixed + lax.dot_general(hidden[1], out_b, NT, preferred_element_type=jnp.float32)
    out_ref[...] = mixed.astype(jnp.bfloat16)


def mix_rows(pieces, x_rows, tables, rotary, where):
    a, b = pieces
    n = a[0].shape[-1]
    length, d = x_rows.shape
    hbm = pl.BlockSpec(memory_space=pltpu.MemorySpace.HBM)
    whole = lambda v: pl.BlockSpec(v.shape, lambda i, w, r=v.ndim: (0,) * r)
    rows = lambda cols: pl.BlockSpec((ROWS, cols), lambda i, w: (i, 0))
    return pl.pallas_call(
        mix_body,
        out_shape=jax.ShapeDtypeStruct((length, d), jnp.bfloat16),
        grid_spec=pltpu.PrefetchScalarGridSpec(
            num_scalar_prefetch=1,
            grid=(length // ROWS,),
            in_specs=[rows(d), rows(DK), rows(DK)] + [whole(t) for t in tables] + [hbm] * 10,
            out_specs=rows(d),
            scratch_shapes=[
                pltpu.VMEM((2, 4, 4, 64, n), jnp.bfloat16),
                pltpu.VMEM((2, 4, 4, 64, n), jnp.bfloat16),
                pltpu.VMEM((2, DK, DV), jnp.float32),
                pltpu.SemaphoreType.DMA((10,)),
            ],
        ),
        compiler_params=pltpu.CompilerParams(vmem_limit_bytes=48 * 2**20),
        name="mix_rows",
    )(where, x_rows, *rotary, *tables, *a, *b)


def ffn_body(x_ref, gate_ref, up_ref, gate_taps, up_taps, out_ref, w):
    half = gate_ref.shape[2]
    w[:, :half] = gate_ref[0]
    w[:, half:] = up_ref[0]
    pre = jnp.dot(x_ref[...], w[...], preferred_element_type=jnp.float32)
    pre = pre.astype(jnp.bfloat16).astype(jnp.float32)
    place = lax.broadcasted_iota(jnp.int32, pre.shape, 0)
    one = jnp.where(place >= 1, pltpu.roll(pre, 1, 0), 0.0)
    two = jnp.where(place >= 2, pltpu.roll(pre, 2, 0), 0.0)
    taps = jnp.concatenate([gate_taps[...], up_taps[...]], axis=1)
    conv = taps[0:1] * two + taps[1:2] * one + taps[2:3] * pre
    gate, up = conv[:, :half], conv[:, half:]
    out_ref[...] = (gate / (1.0 + jnp.exp(-gate)) * up).astype(jnp.bfloat16)


def ffn_rows(x_rows, full, gate_taps, up_taps, first):
    length, d = x_rows.shape
    ff = gate_taps.shape[1]
    tile = 128
    return pl.pallas_call(
        ffn_body,
        out_shape=jax.ShapeDtypeStruct((length, ff), jnp.bfloat16),
        grid=(ff // tile,),
        in_specs=[
            pl.BlockSpec((length, d), lambda j: (0, 0)),
            pl.BlockSpec((1, d, tile), lambda j: (0, 0, first // tile + j)),
            pl.BlockSpec((1, d, tile), lambda j: (1, 0, first // tile + j)),
            pl.BlockSpec((KERNEL, tile), lambda j: (0, j)),
            pl.BlockSpec((KERNEL, tile), lambda j: (0, j)),
        ],
        out_specs=pl.BlockSpec((length, tile), lambda j: (0, j)),
        scratch_shapes=[pltpu.VMEM((d, 2 * tile), jnp.bfloat16)],
        compiler_params=pltpu.CompilerParams(vmem_limit_bytes=40 * 2**20),
        name="ffn_rows",
    )(x_rows, full, full, gate_taps, up_taps)


def down_body(where_ref, act_ref, a_ref, b_ref, out_ref):
    del where_ref
    na = a_ref.shape[2]
    act = act_ref[...]
    total = lax.dot_general(act[:, :na], a_ref[0], NT, preferred_element_type=jnp.float32)
    total = total + lax.dot_general(act[:, na:], b_ref[0], NT, preferred_element_type=jnp.float32)
    out_ref[...] = total.astype(jnp.bfloat16)


def down_rows(activ, full, which, na, nb):
    length, ff = activ.shape
    d = full.shape[1]
    tile = 512
    return pl.pallas_call(
        down_body,
        out_shape=jax.ShapeDtypeStruct((length // 2, d), jnp.bfloat16),
        grid_spec=pltpu.PrefetchScalarGridSpec(
            num_scalar_prefetch=1,
            grid=(d // tile,),
            in_specs=[
                pl.BlockSpec((length // 2, ff), lambda j, w: (w[0], 0)),
                pl.BlockSpec((1, tile, na), lambda j, w: (0, j, 0)),
                pl.BlockSpec((1, tile, nb), lambda j, w: (1, j, 0)),
            ],
            out_specs=pl.BlockSpec((length // 2, tile), lambda j, w: (0, j)),
        ),
        compiler_params=pltpu.CompilerParams(vmem_limit_bytes=32 * 2**20),
        name="down_rows",
    )(which, activ, full, full)


def body(
    tokens,
    mix_gain,
    w_query,
    w_key,
    w_value,
    w_out,
    ffn_gain,
    w_ffgate,
    w_ffup,
    conv_gate,
    conv_up,
    w_down,
):
    tp_rank = lax.axis_index("tp")
    heads_here = w_query.shape[1] // DK
    ff_here = w_ffgate.shape[1]
    na, nb = 768, 640
    down_t = w_down.T
    mine = jnp.where(
        lax.axis_index("rep") == 0,
        jnp.concatenate([down_t[:, :na], w_ffgate], axis=1),
        jnp.concatenate([down_t[:, na:], jnp.zeros((64, na - nb), jnp.bfloat16), w_ffup], axis=1),
    )
    full = lax.all_gather(mine, FULL, axis=0, tiled=True).reshape(2, -1, mine.shape[1])

    out_t = w_out.T
    where = jnp.stack([lax.axis_index(axis) for axis in ("z", "y", "x", "tp")]).astype(jnp.int32)
    wide = jnp.concatenate([w_query, w_key, out_t[:, :DV], w_value, out_t[:, DV:]], axis=1)
    pieces = gather_pieces(wide, wide.shape[1] // 2, where)
    tokens_both = both_rows(tokens, where)
    normed = rms_rows(tokens_both, mix_gain)
    mix = mix_rows(pieces, normed, decay_tables(tp_rank, heads_here), rotary_tables(), where)
    mix_other = shift(mix, "tp", 1)
    mix_sum = mix.astype(jnp.float32) + mix_other.astype(jnp.float32)
    resid = (tokens_both.astype(jnp.float32) + mix_sum).astype(jnp.bfloat16)
    normed_ffn = rms_rows(resid, ffn_gain)
    gate_taps = lax.dynamic_slice_in_dim(conv_gate, tp_rank * ff_here, ff_here, 1)
    up_taps = lax.dynamic_slice_in_dim(conv_up, tp_rank * ff_here, ff_here, 1)
    activ = ffn_rows(normed_ffn, full, gate_taps, up_taps, na)
    me = tp_rank.astype(jnp.int32).reshape(1)
    theirs = down_rows(activ, full, 1 - me, na, nb)
    got = shift(theirs, "tp", 1)
    own = down_rows(activ, full, me, na, nb)
    resid_own = lax.dynamic_slice_in_dim(resid, tp_rank * tokens.shape[0], tokens.shape[0], 0)
    ffn_sum = own.astype(jnp.float32) + got.astype(jnp.float32)
    return (resid_own.astype(jnp.float32) + ffn_sum).astype(jnp.bfloat16)


def solution(mesh):
    torus = Mesh(mesh.devices.reshape(2, 2, 4, 4, 2), ("rep", "z", "y", "x", "tp"))
    fs = ("z", "y", "x")
    rows = P(("rep", *fs, "tp"), None)
    placed = (
        rows,
        P(),
        P(fs, "tp"),
        P(fs, "tp"),
        P(fs, "tp"),
        P("tp", fs),
        P(),
        P(fs, "tp"),
        P(fs, "tp"),
        P(),
        P(),
        P("tp", fs),
    )
    return jax.shard_map(body, mesh=torus, in_specs=placed, out_specs=rows, check_vma=False)
```
